32 devices in a mesh: sp: 8 (over z, y), tp: 4 (over x, core).
Axes of the slice: x: 2, y: 2, z: 4, core: 2. Of those that a mesh axis runs over, the one named last changes fastest.
Arguments:
- tokens: bfloat16 [8192, 4096], P('sp', 'tp'), may hold values from -16 to 16
- norm_gain: float32 [4096], replicated, may hold values from 0.1 to 1.9
- w_pool_in: bfloat16 [4096, 2048], P('sp', 'tp'), may hold values from -0.09375 to 0.09375
- w_query: bfloat16 [4096, 2048], P('sp', 'tp'), may hold values from -0.09375 to 0.09375
- w_key: bfloat16 [4096, 256], P('sp', 'tp'), may hold values from -0.09375 to 0.09375
- w_value: bfloat16 [4096, 256], P('sp', 'tp'), may hold values from -0.09375 to 0.09375
- pool_map: bfloat16 [4, 512, 512], P('tp'), may hold values from -0.25 to 0.25
- pool_scale: float32 [2048], P('tp'), may hold values from 0.3 to 3
- q_gain: float32 [64], replicated, may hold values from 0.1 to 1.9
- k_gain: float32 [64], replicated, may hold values from 0.1 to 1.9
- sinks: float32 [32], P('tp'), may hold values from 0 to 4
- w_out: bfloat16 [4096, 4096], P('tp', 'sp'), may hold values from -0.09375 to 0.09375
Outputs:
- layer_out: bfloat16 [8192, 4096], P(('sp', 'tp'))
The draws below stay inside these ranges and needn't reach their ends.
All inputs are finite; a program needn't handle non-finite values.
Results may differ from the reference program's by a relative error of at most 0.012.
Values may be sent and summed in bfloat16 or wider, within the bound.
No kernel may reach another device: no remote copies, remote signals or barrier semaphores. Data moves between devices by JAX's collectives and lax.ppermute only.
A program may use at most 128 MiB of HBM per device.

```python
import math
import jax
import jax.numpy as jnp
from jax import lax

D = 4096
HEAD_DIM = 64
GROUP = 8
GROUPS = 4
WINDOW = 128
GROUP_WIDTH = 512
Q_HEADS = 32
BRANCH_WIDTH = 2048
MIX = 4096
TOKENS = 8192
N_TP = 4


def draw_tokens(key, part):
    first_key, second_key = jax.random.split(jax.random.fold_in(key, 11), 2)
    base_rows = jnp.clip(jax.random.normal(first_key, (TOKENS, D), jnp.float32), -5.0, 5.0)
    row_scale = jnp.exp(jax.random.uniform(second_key, (TOKENS, 1), jnp.float32, math.log(0.3), math.log(3.0)))
    return (base_rows * row_scale).astype(jnp.bfloat16)


def shard_levels(key, extent, pieces, least, high):
    def one(dim, shards_of):
        steps = jax.random.uniform(jax.random.fold_in(jax.random.fold_in(key, 6), dim), (shards_of,), jnp.float32, least / len(pieces), high / len(pieces))
        return jnp.repeat(jnp.exp(steps), extent[dim] // shards_of).reshape((-1,) + (1,) * (len(extent) - dim - 1))

    level = one(*pieces[0])
    for cut in pieces[1:]:
        level = level * one(*cut)
    return level


def gaussian(own_key, dims, scale, bound, cuts=(), held_as=jnp.bfloat16):
    drawn = jax.random.normal(own_key, dims, jnp.float32) * scale
    if len(cuts) > 0:
        drawn = shard_levels(own_key, dims, cuts, -0.22, 0.18) * drawn
    return jnp.clip(drawn, min=-bound, max=bound).astype(held_as)


def setup_inputs(seed: int = 0) -> dict:
    splits = jax.random.split(jax.random.key(seed), 13)
    return {
        "tokens": draw_tokens(jax.random.fold_in(splits[12], 71), 0),
        "norm_gain": jnp.clip(1.0 + 0.18 * jax.random.normal(splits[1], (D,), jnp.float32), 0.1, 1.9),
        "w_pool_in": gaussian(splits[2], (D, BRANCH_WIDTH), D ** -0.5, 0.09375, ((0, 8), (1, 4))),
        "w_query": gaussian(splits[3], (D, BRANCH_WIDTH), D ** -0.5, 0.09375, ((0, 8), (1, 4))),
        "w_key": gaussian(splits[4], (D, GROUPS * HEAD_DIM), D ** -0.5, 0.09375, ((0, 8), (1, 4))),
        "w_value": gaussian(splits[5], (D, GROUPS * HEAD_DIM), D ** -0.5, 0.09375, ((0, 8), (1, 4))),
        "pool_map": gaussian(splits[6], (GROUPS, GROUP_WIDTH, GROUP_WIDTH), GROUP_WIDTH ** -0.5, 0.25, ((0, 4),)),
        "pool_scale": jnp.clip(jnp.exp(math.log(3.0) - 2.3025851 * jax.random.uniform(splits[7], (BRANCH_WIDTH,), jnp.float32) ** shard_levels(splits[7], (BRANCH_WIDTH,), ((0, 4),), -0.2, 0.2)), 0.3, 3.0),
        "q_gain": jnp.clip(1.0 + 0.18 * jax.random.normal(splits[8], (HEAD_DIM,), jnp.float32), 0.1, 1.9),
        "k_gain": jnp.clip(1.0 + 0.18 * jax.random.normal(splits[9], (HEAD_DIM,), jnp.float32), 0.1, 1.9),
        "sinks": jnp.clip(4.0 * jax.random.uniform(splits[10], (Q_HEADS,), jnp.float32) ** shard_levels(splits[10], (Q_HEADS,), ((0, 4),), -0.2, 0.2), 0.0, 4.0),
        "w_out": gaussian(splits[11], (MIX, D), MIX ** -0.5, 0.09375, ((0, 4), (1, 8))),
    }


epsilon = 1e-06

def rms_scale(values):
    return values * lax.rsqrt(lax.optimization_barrier(jnp.mean(values * values, axis=-1, keepdims=True)) + epsilon)

def reference(tokens, norm_gain, w_pool_in, w_query, w_key, w_value, pool_map, pool_scale, q_gain, k_gain, sinks, w_out):
    widened = tokens.astype(jnp.float32)
    normed = (rms_scale(widened) * norm_gain).astype(jnp.bfloat16)
    pool_in = jnp.dot(normed, w_pool_in, preferred_element_type=jnp.float32).astype(jnp.bfloat16)
    query_rows = jnp.dot(normed, w_query, preferred_element_type=jnp.float32).astype(jnp.bfloat16)
    key_rows = jnp.dot(normed, w_key, preferred_element_type=jnp.float32).astype(jnp.bfloat16)
    value_rows = jnp.dot(normed, w_value, preferred_element_type=jnp.float32).astype(jnp.bfloat16)
    query_float = lax.optimization_barrier(query_rows).astype(jnp.float32).reshape(TOKENS, Q_HEADS, HEAD_DIM)
    query_normed = (rms_scale(query_float) * q_gain).astype(jnp.bfloat16)
    key_float = lax.optimization_barrier(key_rows).astype(jnp.float32).reshape(TOKENS, GROUPS, HEAD_DIM)
    key_normed = (rms_scale(key_float) * k_gain).astype(jnp.bfloat16)
    value_heads = value_rows.reshape(TOKENS, GROUPS, HEAD_DIM)
    positions = jnp.arange(TOKENS, dtype=jnp.int32)
    pool_float = pool_in.astype(jnp.float32).reshape(TOKENS, GROUPS, GROUP_WIDTH)
    padded = jnp.pad(pool_float, ((15, 0), (0, 0), (0, 0)))
    blocks = TOKENS // WINDOW
    key_padded = jnp.concatenate([jnp.zeros((WINDOW, GROUPS, HEAD_DIM), jnp.bfloat16), key_normed], axis=0)
    value_padded = jnp.concatenate([jnp.zeros((WINDOW, GROUPS, HEAD_DIM), jnp.bfloat16), value_heads], axis=0)
    query_pos = jnp.arange(WINDOW, dtype=jnp.int32)[:, None] + WINDOW
    key_pos = jnp.arange(2 * WINDOW, dtype=jnp.int32)[None, :]
    distance = query_pos - key_pos
    in_band = (distance >= 0) & (distance < WINDOW)
    key_global = jnp.arange(blocks, dtype=jnp.int32)[:, None] * WINDOW - WINDOW + jnp.arange(2 * WINDOW, dtype=jnp.int32)[None, :]
    allowed = in_band[None] & (key_global >= 0)[:, None, :]
    branches = []
    for group_index in range(GROUPS):
        span_width = 2 ** (group_index + 1)
        running = jnp.zeros((TOKENS, GROUP_WIDTH), jnp.float32)
        for offset in range(span_width):
            running = running + padded[15 - offset:15 - offset + TOKENS, group_index]
        counts = jnp.minimum(positions.astype(jnp.float32) + 1.0, float(span_width))
        pool_diff = (running / counts[:, None] - pool_float[:, group_index]).astype(jnp.bfloat16)
        mapped = jnp.dot(pool_diff, pool_map[group_index], preferred_element_type=jnp.float32)
        mapped = mapped * pool_scale[group_index * GROUP_WIDTH:(group_index + 1) * GROUP_WIDTH]
        pool_branch = rms_scale(mapped)
        head_first = group_index * GROUP
        query_blocks = query_normed[:, head_first:head_first + GROUP].reshape(blocks, WINDOW, GROUP, HEAD_DIM).astype(jnp.float32)
        key_pairs = jnp.concatenate([key_padded[:TOKENS, group_index].reshape(blocks, WINDOW, HEAD_DIM), key_padded[WINDOW:, group_index].reshape(blocks, WINDOW, HEAD_DIM)], axis=1).astype(jnp.float32)
        value_pairs = jnp.concatenate([value_padded[:TOKENS, group_index].reshape(blocks, WINDOW, HEAD_DIM), value_padded[WINDOW:, group_index].reshape(blocks, WINDOW, HEAD_DIM)], axis=1).astype(jnp.float32)
        scores = jnp.einsum('nqgd,nkd->ngqk', query_blocks, key_pairs) * HEAD_DIM ** (-0.5)
        head_ids = head_first + jnp.arange(GROUP, dtype=jnp.int32) + 1
        slopes = jnp.exp2(-8.0 * head_ids.astype(jnp.float32) / Q_HEADS)
        logits = scores - slopes[None, :, None, None] * distance.astype(jnp.float32)[None, None]
        exp_scores = jnp.exp(jnp.where(allowed[:, None], logits, -jnp.inf))
        sink_logits = sinks[head_first:head_first + GROUP]
        denominator = lax.optimization_barrier(jnp.sum(exp_scores, axis=-1)) + jnp.exp(sink_logits)[None, :, None]
        weights_bf = (exp_scores / denominator[..., None]).astype(jnp.bfloat16)
        attended = jnp.einsum('ngqk,nkd->nqgd', weights_bf.astype(jnp.float32), value_pairs)
        attn_branch = rms_scale(attended.reshape(TOKENS, GROUP_WIDTH))
        branches.append(jnp.stack([pool_branch, attn_branch], axis=1))
    mixed_rows = jnp.stack(branches, axis=1).reshape(TOKENS, MIX).astype(jnp.bfloat16)
    block_width = MIX // N_TP
    summed = jnp.zeros((TOKENS, D), jnp.float32)
    for part_index in range(N_TP):
        row_start = part_index * block_width
        partial_term = jnp.dot(mixed_rows[:, row_start:row_start + block_width], w_out[row_start:row_start + block_width], preferred_element_type=jnp.float32).astype(jnp.bfloat16)
        summed = summed + lax.optimization_barrier(partial_term).astype(jnp.float32)
    return summed.astype(jnp.bfloat16)
```

```python
import jax
import jax.numpy as jnp
from jax import lax
from jax.sharding import PartitionSpec as P

HEAD_DIM = 64
GROUP = 8
WINDOW = 128
GROUP_WIDTH = 512
Q_HEADS = 32
IN_PIECES = 1
OUT_PIECES = 1


epsilon = 1e-06


def passed_along(value, axis, steps):
    count = lax.axis_size(axis)
    first, last = (max(0, -steps), min(count, count - steps))
    return lax.ppermute(value, axis, [(source, source + steps) for source in range(first, last)])


def rms_scale(values):
    return values * lax.rsqrt(jnp.mean(values * values, axis=-1, keepdims=True) + epsilon)


def after(value, *earlier):
    return lax.optimization_barrier((value,) + earlier)[0]


def line_pairs(line, step, direction):
    if direction > 0:
        return [(place, place + 1) for place in range(step - 1, line - 1)]
    return [(place, place - 1) for place in range(line - step, 0, -1)]


def along_line(value, pairs):
    return lax.ppermute(value, "sp", [(2 * s + y, 2 * d + y) for s, d in pairs for y in range(2)])


def across_pair(value, places):
    return lax.ppermute(value, "sp", [(2 * p + y, 2 * p + 1 - y) for p in places for y in range(2)])


def gather_pieces(block, pieces, axis, line_after=(), pair_after=()):
    line = lax.axis_size("sp") // 2
    half = line // 2
    index = lax.axis_index("sp")
    place, side = index // 2, index % 2
    low = place < half
    edge = jnp.minimum(place, line - 1 - place)
    toward = jnp.where(low, 1, -1)
    every = range(line)
    inner = [p for p in every if min(p, line - 1 - p) >= 1]
    ends = [p for p in every if min(p, line - 1 - p) < 1]
    size = block.shape[axis] // pieces
    parts = [lax.slice_in_dim(block, i * size, (i + 1) * size, axis=axis) for i in range(pieces)]
    slots = []
    line_last, pair_last = [], []
    own = [p if not line_after else after(p, *line_after) for p in parts]
    own_pair = [p if not pair_after else after(p, *pair_after) for p in parts]
    other = [across_pair(p, every) for p in own_pair]
    fwd = [{0: p} for p in own]
    bwd = [{0: p} for p in own]
    for step in range(1, half + 1):
        for i in range(pieces):
            fwd[i][step] = along_line(fwd[i][step - 1], line_pairs(line, step, 1))
            bwd[i][step] = along_line(bwd[i][step - 1], line_pairs(line, step, -1))
    near = [{k: jnp.where(low, bwd[i][k], fwd[i][k]) for k in range(1, half + 1)} for i in range(pieces)]
    late = [{half: near[i][half]} for i in range(pieces)]
    for step in range(half + 1, line):
        pairs = line_pairs(line, step, 1) + line_pairs(line, step, -1)
        for i in range(pieces):
            late[i][step] = along_line(late[i][step - 1], pairs)
    from_out = [(p - 1, p) for p in range(1, half)] + [(p + 1, p) for p in range(half, line - 1)]
    to_ends = [(1, 0), (line - 2, line - 1)]
    early_far = [jnp.where(low, fwd[i][1], bwd[i][1]) for i in range(pieces)]
    slots.append((place, side, parts))
    slots.append((place, 1 - side, other))
    for k in range(1, half + 1):
        where = place + toward * k
        slots.append((where, side, [near[i][k] for i in range(pieces)]))
        got = []
        for i in range(pieces):
            if k == 1 and pieces > 1 and i >= (pieces + 1) // 2 and inner:
                mine = across_pair(near[i][k], inner)
                theirs = along_line(after(other[i], late[i][line - 1]), to_ends)
                got.append(jnp.where(edge >= 1, mine, theirs))
            else:
                got.append(across_pair(near[i][k], every))
        slots.append((where, 1 - side, got))
    for m in range(1, half):
        where = jnp.where(edge >= m, place - toward * m, place + toward * (line - m))
        mine, theirs = [], []
        for i in range(pieces):
            early = jnp.where(low, fwd[i][m], bwd[i][m])
            mine.append(jnp.where(edge >= m, early, late[i][line - m]))
            if m == 1:
                early_other = along_line(other[i], from_out)
            else:
                early_other = across_pair(early, [p for p in every if min(p, line - 1 - p) >= m])
            late_other = across_pair(late[i][line - m], [p for p in every if min(p, line - 1 - p) < m])
            theirs.append(jnp.where(edge >= m, early_other, late_other))
            pair_last.append(late_other)
        slots.append((where, side, mine))
        slots.append((where, 1 - side, theirs))
    for i in range(pieces):
        line_last.append(late[i][line - 1])
    found = []
    for where, which, values in slots:
        for i in range(pieces):
            found.append((2 * where + which, i, values[i]))
    return found, line_last, pair_last


def tp_swap(value, bit):
    return lax.ppermute(value, "tp", [(t, t ^ bit) for t in range(lax.axis_size("tp"))])


def gather_features(tokens):
    count, tp_index = lax.axis_size("tp"), lax.axis_index("tp")
    per = lax.axis_size("sp") // count
    rows, width = tokens.shape
    wide = width // per
    blocked = jnp.stack([tokens[:, j * wide : (j + 1) * wide] for j in range(per)])
    held = [(tp_index, blocked)]
    bit = count // 2
    while bit:
        held = held + [(owner ^ bit, tp_swap(value, bit)) for owner, value in held]
        bit //= 2
    whole = jnp.zeros((count * per, rows, wide), tokens.dtype)
    for owner, value in held:
        whole = lax.dynamic_update_slice_in_dim(whole, value, owner * per, axis=0)
    return whole


def scatter_rows(partial):
    count, tp_index = lax.axis_size("tp"), lax.axis_index("tp")
    rows = partial.shape[0] // count
    held = partial.reshape(count, rows, partial.shape[1])
    total = None
    bit = 1
    kept = [held]
    value = held
    while bit < count:
        pairs = value.reshape(-1, 2, rows, partial.shape[1])
        mine_bit = (tp_index // bit) % 2
        away = lax.dynamic_index_in_dim(pairs, 1 - mine_bit, axis=1, keepdims=False)
        mine = lax.dynamic_index_in_dim(pairs, mine_bit, axis=1, keepdims=False)
        came = tp_swap(away.astype(jnp.bfloat16), bit)
        value = mine.astype(jnp.float32) + came.astype(jnp.float32)
        bit *= 2
    return value.reshape(rows, partial.shape[1]).astype(jnp.bfloat16)


def local(
    tokens,
    norm_gain,
    w_pool_in,
    w_query,
    w_key,
    w_value,
    pool_map,
    pool_scale,
    q_gain,
    k_gain,
    sinks,
    w_out,
):
    tok_rows = tokens.shape[0]
    local_groups = w_key.shape[1] // HEAD_DIM
    seq_index = lax.axis_index("sp")
    group_first = lax.axis_index("tp") * local_groups
    w_in = jnp.concatenate([w_pool_in, w_query, w_key, w_value], axis=1)
    in_slots, line_last, pair_last = gather_pieces(w_in, IN_PIECES, 0)
    features = gather_features(tokens)
    widened = features.astype(jnp.float32)
    mean_square = jnp.sum(widened * widened, axis=(0, 2)) / (features.shape[0] * features.shape[2])
    gain = norm_gain.reshape(features.shape[0], 1, features.shape[2])
    normed = (widened * lax.rsqrt(mean_square + epsilon)[None, :, None] * gain).astype(jnp.bfloat16)
    ext_rows = tok_rows
    total = None
    for index, part, weights in in_slots:
        deep = weights.shape[0]
        feats = lax.dynamic_index_in_dim(normed, index, axis=0, keepdims=False)[:, part * deep : (part + 1) * deep]
        term = jnp.dot(feats, weights, preferred_element_type=jnp.float32)
        total = term if total is None else total + term
    pool_wide, query_wide, key_wide = w_pool_in.shape[1], w_query.shape[1], w_key.shape[1]
    pool_sum = total[:, :pool_wide]
    query_sum = total[:, pool_wide : pool_wide + query_wide]
    key_sum = total[:, pool_wide + query_wide : pool_wide + query_wide + key_wide]
    value_sum = total[:, pool_wide + query_wide + key_wide :]
    pool_in = pool_sum.astype(jnp.bfloat16)
    query_rows = lax.optimization_barrier(query_sum.astype(jnp.bfloat16))
    key_rows = lax.optimization_barrier(key_sum.astype(jnp.bfloat16))
    value_rows = value_sum.astype(jnp.bfloat16).reshape(ext_rows, local_groups, HEAD_DIM)
    query_float = query_rows.astype(jnp.float32).reshape(ext_rows, local_groups * GROUP, HEAD_DIM)
    query_normed = (
        (rms_scale(query_float) * q_gain)
        .astype(jnp.bfloat16)
        .reshape(ext_rows, local_groups, GROUP, HEAD_DIM)
    )
    key_float = key_rows.astype(jnp.float32).reshape(ext_rows, local_groups, HEAD_DIM)
    key_normed = (rms_scale(key_float) * k_gain).astype(jnp.bfloat16)
    key_width = local_groups * HEAD_DIM
    pair_tail = jnp.concatenate(
        [
            key_normed[tok_rows - WINDOW :].reshape(WINDOW, key_width),
            value_rows[tok_rows - WINDOW :].reshape(WINDOW, key_width),
        ],
        axis=1,
    )
    earlier_pairs, earlier_pool = passed_along((pair_tail, pool_in[tok_rows - 15 :]), "sp", 1)
    key_span = jnp.concatenate(
        [earlier_pairs[:, :key_width].reshape(WINDOW, local_groups, HEAD_DIM), key_normed], axis=0
    )
    value_span = jnp.concatenate(
        [earlier_pairs[:, key_width:].reshape(WINDOW, local_groups, HEAD_DIM), value_rows], axis=0
    )
    pool_span = jnp.concatenate([earlier_pool, pool_in], axis=0)
    positions = seq_index * tok_rows + jnp.arange(tok_rows, dtype=jnp.int32)
    group_ids = group_first + jnp.arange(local_groups, dtype=jnp.int32)
    spans = jnp.exp2((group_ids + 1).astype(jnp.float32))
    pool_float = pool_span.astype(jnp.float32).reshape(tok_rows + 15, local_groups, GROUP_WIDTH)
    sum_two = pool_float[1:] + pool_float[:-1]
    sum_four = sum_two[2:] + sum_two[:-2]
    sum_eight = sum_four[4:] + sum_four[:-4]
    sum_sixteen = sum_eight[8:] + sum_eight[:-8]
    span_pick = spans[None, :, None]
    running = jnp.where(
        span_pick < 3.0,
        sum_two[14 : 14 + tok_rows],
        jnp.where(
            span_pick < 6.0,
            sum_four[12 : 12 + tok_rows],
            jnp.where(span_pick < 12.0, sum_eight[8 : 8 + tok_rows], sum_sixteen),
        ),
    )
    counts = jnp.minimum(positions.astype(jnp.float32)[:, None] + 1.0, spans[None, :])
    pool_diff = (running / counts[:, :, None] - pool_float[15:]).astype(jnp.bfloat16)
    mapped = jnp.einsum("tlc,lcd->tld", pool_diff, pool_map, preferred_element_type=jnp.float32)
    pool_branch = rms_scale(mapped * pool_scale.reshape(local_groups, GROUP_WIDTH))
    blocks = tok_rows // WINDOW
    query_blocks = query_normed.reshape(blocks, WINDOW, local_groups, GROUP, HEAD_DIM)
    key_pairs = jnp.concatenate(
        [
            key_span[:tok_rows].reshape(blocks, WINDOW, local_groups, HEAD_DIM),
            key_span[WINDOW:].reshape(blocks, WINDOW, local_groups, HEAD_DIM),
        ],
        axis=1,
    )
    value_pairs = jnp.concatenate(
        [
            value_span[:tok_rows].reshape(blocks, WINDOW, local_groups, HEAD_DIM),
            value_span[WINDOW:].reshape(blocks, WINDOW, local_groups, HEAD_DIM),
        ],
        axis=1,
    )
    scores = jnp.einsum(
        "nqlgd,nkld->nlgqk", query_blocks, key_pairs, preferred_element_type=jnp.float32
    ) * HEAD_DIM ** (-0.5)
    query_pos = jnp.arange(WINDOW, dtype=jnp.int32)[:, None] + WINDOW
    key_pos = jnp.arange(2 * WINDOW, dtype=jnp.int32)[None, :]
    distance = query_pos - key_pos
    in_band = (distance >= 0) & (distance < WINDOW)
    key_global = (
        seq_index * tok_rows
        + jnp.arange(blocks, dtype=jnp.int32)[:, None] * WINDOW
        - WINDOW
        + jnp.arange(2 * WINDOW, dtype=jnp.int32)[None, :]
    )
    allowed = in_band[None] & (key_global >= 0)[:, None, :]
    head_ids = group_ids[:, None] * GROUP + jnp.arange(GROUP, dtype=jnp.int32)[None, :] + 1
    slopes = jnp.exp2(-8.0 * head_ids.astype(jnp.float32) / Q_HEADS)
    logits = (
        scores - slopes[None, :, :, None, None] * distance.astype(jnp.float32)[None, None, None]
    )
    exp_scores = jnp.exp(jnp.where(allowed[:, None, None], logits, -jnp.inf))
    sink_logits = sinks.reshape(local_groups, GROUP)
    denominator = jnp.sum(exp_scores, axis=-1) + jnp.exp(sink_logits)[None, :, :, None]
    weights_bf = (exp_scores / denominator[..., None]).astype(jnp.bfloat16)
    attended = jnp.einsum(
        "nlgqk,nkld->nqlgd", weights_bf, value_pairs, preferred_element_type=jnp.float32
    )
    attn_branch = rms_scale(attended.reshape(tok_rows, local_groups, GROUP_WIDTH))
    mixed_rows = (
        jnp.stack([pool_branch, attn_branch], axis=2)
        .reshape(tok_rows, 2 * local_groups * GROUP_WIDTH)
        .astype(jnp.bfloat16)
    )
    out_slots, _, _ = gather_pieces(w_out, OUT_PIECES, 1, line_last, pair_last)
    wide = w_out.shape[1]
    layer_out = jnp.zeros((tok_rows // lax.axis_size("tp"), wide * lax.axis_size("sp")), jnp.bfloat16)
    for index, part, columns in out_slots:
        term = jnp.dot(mixed_rows, columns, preferred_element_type=jnp.float32).astype(jnp.bfloat16)
        layer_out = lax.dynamic_update_slice_in_dim(
            layer_out, scatter_rows(term), index * wide + part * columns.shape[1], axis=1
        )
    return layer_out


def solution(mesh):
    in_specs = (
        P("sp", "tp"),
        P(),
        P("sp", "tp"),
        P("sp", "tp"),
        P("sp", "tp"),
        P("sp", "tp"),
        P("tp", None, None),
        P("tp"),
        P(),
        P(),
        P("tp"),
        P("tp", "sp"),
    )
    out_specs = P(("sp", "tp"), None)
    return jax.shard_map(local, mesh=mesh, in_specs=in_specs, out_specs=out_specs, check_vma=False)
```

```python
import jax
import jax.numpy as jnp
from jax import lax
from jax.sharding import PartitionSpec as P


HEAD_DIM = 64
GROUP = 8
WINDOW = 128
GROUP_WIDTH = 512
Q_HEADS = 32
IN_PIECES = 1
OUT_PIECES = 1


epsilon = 1e-06


def passed_along(value, axis, steps):
    count = lax.axis_size(axis)
    first, last = (max(0, -steps), min(count, count - steps))
    return lax.ppermute(value, axis, [(source, source + steps) for source in range(first, last)])


def rms_scale(values):
    return values * lax.rsqrt(jnp.mean(values * values, axis=-1, keepdims=True) + epsilon)


def after(value, *earlier):
    return lax.optimization_barrier((value,) + earlier)[0]


def line_pairs(line, step, direction):
    if direction > 0:
        return [(place, place + 1) for place in range(step - 1, line - 1)]
    return [(place, place - 1) for place in range(line - step, 0, -1)]


def along_line(value, pairs):
    return lax.ppermute(value, "sp", [(2 * s + y, 2 * d + y) for s, d in pairs for y in range(2)])


def across_pair(value, places):
    return lax.ppermute(value, "sp", [(2 * p + y, 2 * p + 1 - y) for p in places for y in range(2)])


def gather_pieces(block, pieces, axis, line_after=(), pair_after=()):
    line = lax.axis_size("sp") // 2
    half = line // 2
    index = lax.axis_index("sp")
    place, side = index // 2, index % 2
    low = place < half
    edge = jnp.minimum(place, line - 1 - place)
    toward = jnp.where(low, 1, -1)
    every = range(line)
    inner = [p for p in every if min(p, line - 1 - p) >= 1]
    size = block.shape[axis] // pieces
    parts = [lax.slice_in_dim(block, i * size, (i + 1) * size, axis=axis) for i in range(pieces)]
    slots = []
    line_last, pair_last = [], []
    own = [p if not line_after else after(p, *line_after) for p in parts]
    own_pair = [p if not pair_after else after(p, *pair_after) for p in parts]
    other = [across_pair(p, every) for p in own_pair]
    fwd = [{0: p} for p in own]
    bwd = [{0: p} for p in own]
    for step in range(1, half + 1):
        for i in range(pieces):
            fwd[i][step] = along_line(fwd[i][step - 1], line_pairs(line, step, 1))
            bwd[i][step] = along_line(bwd[i][step - 1], line_pairs(line, step, -1))
    near = [{k: jnp.where(low, bwd[i][k], fwd[i][k]) for k in range(1, half + 1)} for i in range(pieces)]
    late = [{half: near[i][half]} for i in range(pieces)]
    for step in range(half + 1, line):
        pairs = line_pairs(line, step, 1) + line_pairs(line, step, -1)
        for i in range(pieces):
            late[i][step] = along_line(late[i][step - 1], pairs)
    from_out = [(p - 1, p) for p in range(1, half)] + [(p + 1, p) for p in range(half, line - 1)]
    to_ends = [(1, 0), (line - 2, line - 1)]
    early_far = [jnp.where(low, fwd[i][1], bwd[i][1]) for i in range(pieces)]
    slots.append((place, side, parts))
    slots.append((place, 1 - side, other))
    for k in range(1, half + 1):
        where = place + toward * k
        slots.append((where, side, [near[i][k] for i in range(pieces)]))
        got = []
        for i in range(pieces):
            if k == 1 and pieces > 1 and i >= (pieces + 1) // 2 and inner:
                mine = across_pair(near[i][k], inner)
                theirs = along_line(after(other[i], late[i][line - 1]), to_ends)
                got.append(jnp.where(edge >= 1, mine, theirs))
            else:
                got.append(across_pair(near[i][k], every))
        slots.append((where, 1 - side, got))
    for m in range(1, half):
        where = jnp.where(edge >= m, place - toward * m, place + toward * (line - m))
        mine, theirs = [], []
        for i in range(pieces):
            early = jnp.where(low, fwd[i][m], bwd[i][m])
            mine.append(jnp.where(edge >= m, early, late[i][line - m]))
            if m == 1:
                early_other = along_line(other[i], from_out)
            else:
                early_other = across_pair(early, [p for p in every if min(p, line - 1 - p) >= m])
            late_other = across_pair(late[i][line - m], [p for p in every if min(p, line - 1 - p) < m])
            theirs.append(jnp.where(edge >= m, early_other, late_other))
            pair_last.append(late_other)
        slots.append((where, side, mine))
        slots.append((where, 1 - side, theirs))
    for i in range(pieces):
        line_last.append(late[i][line - 1])
    found = []
    for where, which, values in slots:
        for i in range(pieces):
            found.append((2 * where + which, i, values[i]))
    return found, line_last, pair_last, near[0][half]


def tp_swap(value, bit):
    return lax.ppermute(value, "tp", [(t, t ^ bit) for t in range(lax.axis_size("tp"))])


def gather_features(tokens, first):
    count, tp_index = lax.axis_size("tp"), lax.axis_index("tp")
    per = lax.axis_size("sp") // count
    rows, width = tokens.shape
    wide = width // per
    blocked = jnp.stack([tokens[:, j * wide : (j + 1) * wide] for j in range(per)])
    held = [(tp_index, blocked)]
    bit = count // 2
    while bit:
        came = [(owner ^ bit, tp_swap(value, bit)) for owner, value in held]
        if bit == count // 2:
            came = [(owner, after(value, first)) for owner, value in came]
        held = held + came
        bit //= 2
    whole = jnp.zeros((count * per, rows, wide), tokens.dtype)
    for owner, value in held:
        whole = lax.dynamic_update_slice_in_dim(whole, value, owner * per, axis=0)
    return whole


def scatter_rows(partial):
    count, tp_index = lax.axis_size("tp"), lax.axis_index("tp")
    rows = partial.shape[0] // count
    held = partial.reshape(count, rows, partial.shape[1])
    bit = 1
    value = held
    while bit < count:
        pairs = value.reshape(-1, 2, rows, partial.shape[1])
        mine_bit = (tp_index // bit) % 2
        away = lax.dynamic_index_in_dim(pairs, 1 - mine_bit, axis=1, keepdims=False)
        mine = lax.dynamic_index_in_dim(pairs, mine_bit, axis=1, keepdims=False)
        came = tp_swap(away.astype(jnp.bfloat16), bit)
        value = mine.astype(jnp.float32) + came.astype(jnp.float32)
        bit *= 2
    return value.reshape(rows, partial.shape[1]).astype(jnp.bfloat16)


def local(
    tokens,
    norm_gain,
    w_pool_in,
    w_query,
    w_key,
    w_value,
    pool_map,
    pool_scale,
    q_gain,
    k_gain,
    sinks,
    w_out,
):
    tok_rows = tokens.shape[0]
    local_groups = w_key.shape[1] // HEAD_DIM
    seq_index = lax.axis_index("sp")
    group_first = lax.axis_index("tp") * local_groups
    w_in = jnp.concatenate([w_pool_in, w_query, w_key, w_value], axis=1)
    in_slots, line_last, pair_last, midway = gather_pieces(w_in, IN_PIECES, 0)
    reach = passed_along(tokens[tok_rows - WINDOW :], "sp", 1)
    features = gather_features(jnp.concatenate([reach, tokens], axis=0), midway)
    widened = features.astype(jnp.float32)
    mean_square = jnp.sum(widened * widened, axis=(0, 2)) / (features.shape[0] * features.shape[2])
    gain = norm_gain.reshape(features.shape[0], 1, features.shape[2])
    normed = (widened * lax.rsqrt(mean_square + epsilon)[None, :, None] * gain).astype(jnp.bfloat16)
    ext_rows = normed.shape[1]
    total = None
    for index, part, weights in in_slots:
        deep = weights.shape[0]
        feats = lax.dynamic_index_in_dim(normed, index, axis=0, keepdims=False)[:, part * deep : (part + 1) * deep]
        term = jnp.dot(feats, weights, preferred_element_type=jnp.float32)
        total = term if total is None else total + term
    pool_wide, query_wide, key_wide = w_pool_in.shape[1], w_query.shape[1], w_key.shape[1]
    pool_sum = total[:, :pool_wide]
    query_sum = total[:, pool_wide : pool_wide + query_wide]
    key_sum = total[:, pool_wide + query_wide : pool_wide + query_wide + key_wide]
    value_sum = total[:, pool_wide + query_wide + key_wide :]
    pool_in = pool_sum.astype(jnp.bfloat16)
    query_rows = lax.optimization_barrier(query_sum[ext_rows - tok_rows :].astype(jnp.bfloat16))
    key_rows = lax.optimization_barrier(key_sum.astype(jnp.bfloat16))
    value_rows = value_sum.astype(jnp.bfloat16).reshape(ext_rows, local_groups, HEAD_DIM)
    query_float = query_rows.astype(jnp.float32).reshape(tok_rows, local_groups * GROUP, HEAD_DIM)
    query_normed = (
        (rms_scale(query_float) * q_gain)
        .astype(jnp.bfloat16)
        .reshape(tok_rows, local_groups, GROUP, HEAD_DIM)
    )
    key_float = key_rows.astype(jnp.float32).reshape(ext_rows, local_groups, HEAD_DIM)
    key_normed = (rms_scale(key_float) * k_gain).astype(jnp.bfloat16)
    key_span, value_span = key_normed, value_rows
    pool_span = pool_in[ext_rows - tok_rows - 15 :]
    positions = seq_index * tok_rows + jnp.arange(tok_rows, dtype=jnp.int32)
    group_ids = group_first + jnp.arange(local_groups, dtype=jnp.int32)
    spans = jnp.exp2((group_ids + 1).astype(jnp.float32))
    pool_float = pool_span.astype(jnp.float32).reshape(tok_rows + 15, local_groups, GROUP_WIDTH)
    sum_two = pool_float[1:] + pool_float[:-1]
    sum_four = sum_two[2:] + sum_two[:-2]
    sum_eight = sum_four[4:] + sum_four[:-4]
    sum_sixteen = sum_eight[8:] + sum_eight[:-8]
    span_pick = spans[None, :, None]
    running = jnp.where(
        span_pick < 3.0,
        sum_two[14 : 14 + tok_rows],
        jnp.where(
            span_pick < 6.0,
            sum_four[12 : 12 + tok_rows],
            jnp.where(span_pick < 12.0, sum_eight[8 : 8 + tok_rows], sum_sixteen),
        ),
    )
    counts = jnp.minimum(positions.astype(jnp.float32)[:, None] + 1.0, spans[None, :])
    pool_diff = (running / counts[:, :, None] - pool_float[15:]).astype(jnp.bfloat16)
    mapped = jnp.einsum("tlc,lcd->tld", pool_diff, pool_map, preferred_element_type=jnp.float32)
    pool_branch = rms_scale(mapped * pool_scale.reshape(local_groups, GROUP_WIDTH))
    blocks = tok_rows // WINDOW
    query_blocks = query_normed.reshape(blocks, WINDOW, local_groups, GROUP, HEAD_DIM)
    key_pairs = jnp.concatenate(
        [
            key_span[:tok_rows].reshape(blocks, WINDOW, local_groups, HEAD_DIM),
            key_span[WINDOW:].reshape(blocks, WINDOW, local_groups, HEAD_DIM),
        ],
        axis=1,
    )
    value_pairs = jnp.concatenate(
        [
            value_span[:tok_rows].reshape(blocks, WINDOW, local_groups, HEAD_DIM),
            value_span[WINDOW:].reshape(blocks, WINDOW, local_groups, HEAD_DIM),
        ],
        axis=1,
    )
    scores = jnp.einsum(
        "nqlgd,nkld->nlgqk", query_blocks, key_pairs, preferred_element_type=jnp.float32
    ) * HEAD_DIM ** (-0.5)
    query_pos = jnp.arange(WINDOW, dtype=jnp.int32)[:, None] + WINDOW
    key_pos = jnp.arange(2 * WINDOW, dtype=jnp.int32)[None, :]
    distance = query_pos - key_pos
    in_band = (distance >= 0) & (distance < WINDOW)
    key_global = (
        seq_index * tok_rows
        + jnp.arange(blocks, dtype=jnp.int32)[:, None] * WINDOW
        - WINDOW
        + jnp.arange(2 * WINDOW, dtype=jnp.int32)[None, :]
    )
    allowed = in_band[None] & (key_global >= 0)[:, None, :]
    head_ids = group_ids[:, None] * GROUP + jnp.arange(GROUP, dtype=jnp.int32)[None, :] + 1
    slopes = jnp.exp2(-8.0 * head_ids.astype(jnp.float32) / Q_HEADS)
    logits = (
        scores - slopes[None, :, :, None, None] * distance.astype(jnp.float32)[None, None, None]
    )
    exp_scores = jnp.exp(jnp.where(allowed[:, None, None], logits, -jnp.inf))
    sink_logits = sinks.reshape(local_groups, GROUP)
    denominator = jnp.sum(exp_scores, axis=-1) + jnp.exp(sink_logits)[None, :, :, None]
    weights_bf = (exp_scores / denominator[..., None]).astype(jnp.bfloat16)
    attended = jnp.einsum(
        "nlgqk,nkld->nqlgd", weights_bf, value_pairs, preferred_element_type=jnp.float32
    )
    attn_branch = rms_scale(attended.reshape(tok_rows, local_groups, GROUP_WIDTH))
    mixed_rows = (
        jnp.stack([pool_branch, attn_branch], axis=2)
        .reshape(tok_rows, 2 * local_groups * GROUP_WIDTH)
        .astype(jnp.bfloat16)
    )
    out_slots = gather_pieces(w_out, OUT_PIECES, 1, line_last, pair_last)[0]
    wide = w_out.shape[1]
    layer_out = jnp.zeros((tok_rows // lax.axis_size("tp"), wide * lax.axis_size("sp")), jnp.bfloat16)
    for index, part, columns in out_slots:
        term = jnp.dot(mixed_rows, columns, preferred_element_type=jnp.float32).astype(jnp.bfloat16)
        layer_out = lax.dynamic_update_slice_in_dim(
            layer_out, scatter_rows(term), index * wide + part * columns.shape[1], axis=1
        )
    return layer_out


def solution(mesh):
    in_specs = (
        P("sp", "tp"),
        P(),
        P("sp", "tp"),
        P("sp", "tp"),
        P("sp", "tp"),
        P("sp", "tp"),
        P("tp", None, None),
        P("tp"),
        P(),
        P(),
        P("tp"),
        P("tp", "sp"),
    )
    out_specs = P(("sp", "tp"), None)

    return jax.shard_map(local, mesh=mesh, in_specs=in_specs, out_specs=out_specs, check_vma=False)
```
